32 devices in a mesh: grp: 2 (over x), sp: 8 (over z, y), tp: 2 (over core).
Axes of the slice: x: 2, y: 2, z: 4, core: 2. Of those that a mesh axis runs over, the one named last changes fastest.
Arguments:
- gate_in: bfloat16 [6144, 2048], P(('grp', 'sp'), 'tp'), parts along dimension 0, may hold values from -6 to 6
- values_in: bfloat16 [6144, 2048], P(('grp', 'sp'), 'tp'), parts along dimension 0, may hold values from -6 to 6
- input_state_in: bfloat16 [6144, 512], P(('grp', 'sp'), 'tp'), parts along dimension 0, may hold values from -6 to 6
- output_state_in: bfloat16 [6144, 512], P(('grp', 'sp'), 'tp'), parts along dimension 0, may hold values from -6 to 6
- step_in: bfloat16 [6144, 32], P(('grp', 'sp'), 'tp'), parts along dimension 0, may hold values from -6 to 6
- conv_x: bfloat16 [4, 2048], P(None, 'tp'), may hold values from -3 to 3
- conv_b: bfloat16 [4, 512], P(None, 'tp'), may hold values from -3 to 3
- conv_c: bfloat16 [4, 512], P(None, 'tp'), may hold values from -3 to 3
- dt_bias: float32 [32], P('tp'), may hold values from -1 to 1
- decay_rate: float32 [32], P('tp'), may hold values from 0 to 1, as said below
- log_decay_extra: float32 [6144, 32], P(('grp', 'sp'), 'tp'), parts along dimension 0, may hold values from -1 to 0
- out_gain: bfloat16 [2048], P('tp'), may hold values from 0.099609375 to 1.8984375
- w_out: bfloat16 [2048, 2048], P('tp'), may hold values from -0.125 to 0.125
Outputs:
- mixed: bfloat16 [6144, 2048], P(('grp', 'sp', 'tp')), parts along dimension 0
The draws below stay inside these ranges and needn't reach their ends.
There are 2 independent parts, one for each index of `grp`. The reference program is written for one: setup_inputs(seed, part) draws one part's arguments, and reference() takes and returns one part's arrays. A program takes and returns all parts, laid end to end along the dimension named above; an argument that names none is the same for every part. Nothing has to cross between parts.
Inputs may be any that keep to these rules, and one draw needn't show every extreme that they name: `decay_rate`: positive rates.
All inputs are finite; a program needn't handle non-finite values.
Results may differ from the reference program's by a relative error of at most 0.01.
Values may be sent and summed in bfloat16 or wider, within the bound.
A program may use at most 128 MiB of HBM per device.

```python
import math
import jax
import jax.numpy as jnp
from jax import lax

D = 2048
MIXER_HEADS = 32
HEAD_DIM = 64
STATE = 128
GROUPS = 4
CONV = 4
BLOCK = 128
DEV_ROWS = 384
SEQUENCE_LENGTH = 3072
D_SSD = 2048


def draw_decay_rate(key, part):
    key_entries = jax.random.split(jax.random.fold_in(key, 11), 3)
    order = jax.random.permutation(key_entries[0], MIXER_HEADS)
    fast = order < MIXER_HEADS // 2
    slow_rate = jax.random.uniform(key_entries[1], (MIXER_HEADS,), jnp.float32, 0.3, 0.6) / SEQUENCE_LENGTH
    fast_rate = jnp.exp(jax.random.uniform(key_entries[2], (MIXER_HEADS,), jnp.float32, math.log(0.02), math.log(0.05)))
    return jnp.where(fast, fast_rate, slow_rate).astype(jnp.float32)


def draw_log_decay_extra(key, part):
    key_entries = jax.random.split(jax.random.fold_in(key, 23), 3)
    spans = SEQUENCE_LENGTH // DEV_ROWS
    factor = jnp.exp(jax.random.uniform(key_entries[0], (spans,), jnp.float32, math.log(0.1), math.log(1.5))) / SEQUENCE_LENGTH
    each_row_count = -jnp.repeat(factor, DEV_ROWS)
    group_token_rows = jax.random.randint(key_entries[1], (2,), 0, SEQUENCE_LENGTH)
    group_span_size = jax.random.uniform(key_entries[2], (2, MIXER_HEADS), jnp.float32, 0.2, 0.4)
    token_positions = jnp.arange(SEQUENCE_LENGTH)
    match_count = (token_positions[:, None] == group_token_rows[None, :]).astype(jnp.float32)
    token_groups = jnp.dot(match_count, jnp.log(1.0 - group_span_size), precision=jax.lax.Precision.HIGHEST)
    return (each_row_count[:, None] + token_groups).astype(jnp.float32)


def block_scale(stream_key, extent, cuts, low, high):
    level = 1.0
    for dim, parts in cuts:
        steps = jax.random.uniform(jax.random.fold_in(jax.random.fold_in(stream_key, 6), dim), (parts,), jnp.float32, low / len(cuts), high / len(cuts))
        level = level * jnp.repeat(jnp.exp(steps), extent[dim] // parts).reshape((-1,) + (1,) * (len(extent) - 1 - dim))
    return level


def centred(stream_key, extent, width, reach, cuts=(), kind=jnp.bfloat16):
    factor_of = block_scale(stream_key, extent, cuts, -0.22, 0.18) if cuts else 1.0
    drawn = jax.random.normal(stream_key, extent, jnp.float32) * width * factor_of
    return jnp.minimum(jnp.maximum(drawn, -reach), reach).astype(kind)


def setup_inputs(seed: int = 0, part: int = 0) -> dict:
    keys = jax.random.split(jax.random.key(seed), 14)
    part_splits = jax.random.split(jax.random.fold_in(keys[13], part), 14)
    return {
        "gate_in": centred(part_splits[0], (SEQUENCE_LENGTH, D_SSD), 1.0, 6.0, ((0, 8), (1, 2))),
        "values_in": centred(part_splits[1], (SEQUENCE_LENGTH, D_SSD), 1.0, 6.0, ((0, 8), (1, 2))),
        "input_state_in": centred(part_splits[2], (SEQUENCE_LENGTH, GROUPS * STATE), 1.0, 6.0, ((0, 8), (1, 2))),
        "output_state_in": centred(part_splits[3], (SEQUENCE_LENGTH, GROUPS * STATE), 1.0, 6.0, ((0, 8), (1, 2))),
        "step_in": centred(part_splits[4], (SEQUENCE_LENGTH, MIXER_HEADS), 1.0, 6.0, ((0, 8), (1, 2))),
        "conv_x": centred(keys[5], (CONV, D_SSD), CONV ** -0.5, 3.0, ((1, 2),)),
        "conv_b": centred(keys[6], (CONV, GROUPS * STATE), CONV ** -0.5, 3.0, ((1, 2),)),
        "conv_c": centred(keys[7], (CONV, GROUPS * STATE), CONV ** -0.5, 3.0, ((1, 2),)),
        "dt_bias": jnp.clip(jax.random.uniform(keys[8], (MIXER_HEADS,), jnp.float32, -1.0, 1.0) * block_scale(keys[8], (MIXER_HEADS,), ((0, 2),), -0.4, 0.0), -1.0, 1.0),
        "decay_rate": draw_decay_rate(jax.random.fold_in(keys[13], 71), part),
        "log_decay_extra": draw_log_decay_extra(jax.random.fold_in(jax.random.fold_in(keys[13], part), 71), part),
        "out_gain": jnp.clip(1.0 + 0.18 * jax.random.normal(keys[11], (D_SSD,), jnp.float32), 0.099609375, 1.8984375).astype(jnp.bfloat16),
        "w_out": centred(keys[12], (D_SSD, D), D_SSD ** -0.5, 0.125, ((0, 2),)),
    }


def rms_rows(values, gain, epsilon):
    floats = values.astype(jnp.float32)
    scaled = floats * lax.rsqrt(lax.optimization_barrier(jnp.mean(floats * floats, axis=-1, keepdims=True)) + epsilon)
    return scaled * gain.astype(jnp.float32)

def conv_silu(signal, kernel):
    length = signal.shape[0]
    padded = jnp.concatenate([jnp.zeros((CONV - 1, signal.shape[1]), jnp.bfloat16), signal], axis=0)
    summed = jnp.zeros(signal.shape, jnp.float32)
    for offset in range(CONV):
        summed = summed + kernel[offset].astype(jnp.float32) * padded[offset:offset + length].astype(jnp.float32)
    return jax.nn.silu(summed).astype(jnp.bfloat16)

def reference(gate_in, values_in, input_state_in, output_state_in, step_in, conv_x, conv_b, conv_c, dt_bias, decay_rate, log_decay_extra, out_gain, w_out):
    x_input = conv_silu(values_in, conv_x)
    b_input = conv_silu(input_state_in, conv_b)
    c_input = conv_silu(output_state_in, conv_c)
    step_size = jax.nn.softplus(step_in.astype(jnp.float32) + dt_bias.astype(jnp.float32))
    log_step = log_decay_extra.astype(jnp.float32) - step_size * decay_rate.astype(jnp.float32)
    per_group = MIXER_HEADS // GROUPS
    count = SEQUENCE_LENGTH // BLOCK
    lower = jnp.tril(jnp.ones((BLOCK, BLOCK), dtype=bool))

    def one_block(state, inputs):
        x_blk, b_blk, c_blk, step_blk, log_blk = inputs
        cum_log = jnp.cumsum(log_blk, axis=0)
        cum_rows = cum_log.T
        scores = jnp.einsum('ign,jgn->gij', c_blk.astype(jnp.float32), b_blk.astype(jnp.float32))
        head_scores = jnp.repeat(scores, per_group, axis=0)
        decay = jnp.exp(jnp.where(lower, cum_rows[:, :, None] - cum_rows[:, None, :], -jnp.inf))
        mixing = (head_scores * decay * step_blk.T[:, None, :]).astype(jnp.bfloat16)
        y_diag = jnp.einsum('hij,jhp->ihp', mixing.astype(jnp.float32), x_blk.astype(jnp.float32))
        to_end = jnp.exp(cum_rows[:, -1:] - cum_rows) * step_blk.T
        b_heads = (jnp.repeat(b_blk.astype(jnp.float32), per_group, axis=1) * to_end.T[:, :, None]).astype(jnp.bfloat16)
        added = jnp.einsum('jhp,jhn->hpn', x_blk.astype(jnp.float32), b_heads.astype(jnp.float32))
        c_heads = jnp.repeat(c_blk.astype(jnp.float32), per_group, axis=1)
        y_state = jnp.einsum('ihn,hpn->ihp', c_heads, state, precision=lax.Precision.HIGHEST) * jnp.exp(cum_log)[:, :, None]
        next_state = state * jnp.exp(cum_rows[:, -1])[:, None, None] + added
        return (next_state, y_diag + y_state)
    initial = jnp.zeros((MIXER_HEADS, HEAD_DIM, STATE), jnp.float32)
    inputs = (x_input.reshape(count, BLOCK, MIXER_HEADS, HEAD_DIM), b_input.reshape(count, BLOCK, GROUPS, STATE), c_input.reshape(count, BLOCK, GROUPS, STATE), step_size.reshape(count, BLOCK, MIXER_HEADS), log_step.reshape(count, BLOCK, MIXER_HEADS))
    _, outputs = lax.scan(one_block, initial, inputs)
    mixed_heads = outputs.reshape(SEQUENCE_LENGTH, MIXER_HEADS, HEAD_DIM)
    gated = mixed_heads * jax.nn.silu(gate_in.astype(jnp.float32)).reshape(SEQUENCE_LENGTH, MIXER_HEADS, HEAD_DIM)
    normalized = rms_rows(gated, out_gain.reshape(MIXER_HEADS, HEAD_DIM), 1e-05).astype(jnp.bfloat16).reshape(SEQUENCE_LENGTH, MIXER_HEADS * HEAD_DIM)
    return jnp.dot(normalized, w_out, preferred_element_type=jnp.float32).astype(jnp.bfloat16)
```

```python
import functools

import jax
import jax.numpy as jnp
from jax import lax
from jax.experimental import pallas as pl
from jax.experimental.pallas import tpu as pltpu
from jax.sharding import PartitionSpec as P

HEAD_DIM = 64
STATE = 128
CONV = 4
BLOCK = 128
HALO = 16
CHUNKS = 4
LANES = 128
WIDE = 256
MESH = pl.DeviceIdType.MESH
F32 = jnp.float32
BF16 = jnp.bfloat16


def silu(v):
    return v / (1.0 + jnp.exp(-v))


def split(v):
    high = v.astype(BF16)
    return high, (v - high.astype(F32)).astype(BF16)


def spread(v, table):
    high, low = split(v)
    return jnp.dot(high, table, preferred_element_type=F32) + jnp.dot(
        low, table, preferred_element_type=F32
    )


def kernel(
    n,
    gate_ref,
    values_ref,
    b_ref,
    c_ref,
    step_ref,
    kx_ref,
    kb_ref,
    kc_ref,
    bias_ref,
    rate_ref,
    extra_ref,
    gain_ref,
    w_ref,
    out_ref,
    stage,
    act,
    weight,
    table,
    to_end,
    growth,
    cum_scr,
    cum_t,
    added,
    y_diag,
    gate_act,
    grown,
    decays,
    message,
    pair_in,
    state_in,
    state_out,
    partner_out,
    carried,
    normed,
    part_out,
    part_in,
    load_sem,
    halo_send,
    halo_recv,
    m1_send,
    m1_recv,
    m2_send,
    m2_recv,
    m3_send,
    m3_recv,
    tp_send,
    tp_recv,
):
    sp = lax.axis_index("sp")
    tp = lax.axis_index("tp")
    place = sp % 2
    pair = sp // 2
    pairs = n // 2
    span, inner = gate_ref.shape
    shared = b_ref.shape[1]
    count = span // BLOCK
    heads = inner // HEAD_DIM
    half = inner // 2
    rows_out, width = out_ref.shape
    pieces = width // WIDE

    loads = [
        pltpu.make_async_copy(values_ref, stage.at[pl.ds(HALO, span), pl.ds(0, inner)], load_sem.at[0]),
        pltpu.make_async_copy(b_ref, stage.at[pl.ds(HALO, span), pl.ds(inner, shared)], load_sem.at[1]),
        pltpu.make_async_copy(
            c_ref, stage.at[pl.ds(HALO, span), pl.ds(inner + shared, shared)], load_sem.at[2]
        ),
        pltpu.make_async_copy(w_ref, weight, load_sem.at[3]),
    ]
    for load in loads:
        load.start()

    barrier = pltpu.get_barrier_semaphore()
    for distance in (1, 2):

        @pl.when(sp >= distance)
        def _():
            pl.semaphore_signal(barrier, inc=1, device_id={"sp": sp - distance}, device_id_type=MESH)

        @pl.when(sp + distance < n)
        def _():
            pl.semaphore_signal(barrier, inc=1, device_id={"sp": sp + distance}, device_id_type=MESH)

    pl.semaphore_signal(barrier, inc=1, device_id={"tp": 1 - tp}, device_id_type=MESH)
    peers = 1
    for distance in (1, 2):
        peers = peers + jnp.where(sp >= distance, 1, 0) + jnp.where(sp + distance < n, 1, 0)
    pl.semaphore_wait(barrier, peers)

    halos = []
    for i, (source, start, size) in enumerate(
        ((values_ref, 0, inner), (b_ref, inner, shared), (c_ref, inner + shared, shared))
    ):
        halos.append(
            pltpu.make_async_remote_copy(
                src_ref=source.at[pl.ds(span - HALO, HALO), :],
                dst_ref=stage.at[pl.ds(0, HALO), pl.ds(start, size)],
                send_sem=halo_send.at[i],
                recv_sem=halo_recv.at[i],
                device_id={"sp": jnp.minimum(sp + 1, n - 1)},
                device_id_type=MESH,
            )
        )

    @pl.when(sp + 1 < n)
    def _():
        for copy in halos:
            copy.start()

    @pl.when(sp == 0)
    def _():
        stage[pl.ds(0, HALO), :] = jnp.zeros((HALO, stage.shape[1]), BF16)

    head_of = lax.broadcasted_iota(jnp.int32, (heads, inner), 1) // HEAD_DIM
    row_of = lax.broadcasted_iota(jnp.int32, (heads, inner), 0)
    table[...] = jnp.where(head_of == row_of, 1.0, 0.0).astype(BF16)
    step = jax.nn.softplus(step_ref[...].astype(F32) + bias_ref[...])
    log_step = extra_ref[...] - step * rate_ref[...]
    ri = lax.broadcasted_iota(jnp.int32, (BLOCK, BLOCK), 0)
    ci = lax.broadcasted_iota(jnp.int32, (BLOCK, BLOCK), 1)
    lower = jnp.where(ri >= ci, 1.0, 0.0).astype(F32)
    totals = []
    for blk in range(count):
        rows = slice(blk * BLOCK, (blk + 1) * BLOCK)
        cum = jnp.dot(lower, log_step[rows], precision=lax.Precision.HIGHEST, preferred_element_type=F32)
        last = cum[BLOCK - 1 :, :]
        totals.append(jnp.exp(last))
        to_end[rows, :] = jnp.exp(last - cum) * step[rows]
        growth[rows, :] = jnp.exp(cum)
        cum_scr[rows, :] = cum
        wide = jnp.concatenate(
            [cum, step[rows], jnp.zeros((BLOCK, LANES - 2 * heads), F32)], axis=1
        )
        cum_t[blk] = wide.T[: 2 * heads, :]
    stacked = jnp.concatenate(totals + [jnp.zeros((8 - count, heads), F32)], axis=0)
    decays[...] = spread(stacked, table[...])

    def conv_tile(blk, taps_ref, column, offset):
        rows = pl.ds(pl.multiple_of(blk * BLOCK, BLOCK), BLOCK + HALO)
        window = stage[rows, pl.ds(pl.multiple_of(offset + column, LANES), LANES)].astype(F32)
        taps = taps_ref[:, pl.ds(column, LANES)].astype(F32)
        total = taps[CONV - 1 :, :] * window[HALO:]
        for j in range(CONV - 1):
            total = total + taps[j : j + 1, :] * pltpu.roll(window, CONV - 1 - j, axis=0)[HALO:]
        out_rows = pl.ds(pl.multiple_of(blk * BLOCK, BLOCK), BLOCK)
        act[out_rows, pl.ds(pl.multiple_of(offset + column, LANES), LANES)] = silu(total).astype(BF16)

    def early(blk):
        rows = pl.ds(pl.multiple_of(blk * BLOCK, BLOCK), BLOCK)
        for t in range(shared // LANES):
            conv_tile(blk, kb_ref, t * LANES, inner)
        for t in range(inner // LANES):
            conv_tile(blk, kx_ref, t * LANES, 0)
        ends_high, ends_low = split(to_end[rows, :])
        per = inner // (shared // STATE)
        for g in range(shared // STATE):
            b_blk = act[rows, pl.ds(inner + g * STATE, STATE)].astype(F32).T.astype(BF16)
            for t in range(per // WIDE):
                cols = pl.ds(g * per + t * WIDE, WIDE)
                scale = jnp.dot(ends_high, table[:, cols], preferred_element_type=F32) + jnp.dot(
                    ends_low, table[:, cols], preferred_element_type=F32
                )
                weighted = (act[rows, cols].astype(F32) * scale).astype(BF16)
                added[blk, :, cols] = jnp.dot(b_blk, weighted, preferred_element_type=F32)

    for i in range(3):
        loads[i].wait()

    @pl.loop(0, count - 1)
    def _(i):
        early(count - 1 - i)

    @pl.when(sp > 0)
    def _():
        for copy in halos:
            copy.wait_recv()

    @pl.loop(0, 1)
    def _(i):
        early(i)

    decay_all = decays[0:1, :]
    for blk in range(1, count):
        decay_all = decay_all * decays[blk : blk + 1, :]
    for s in range(2):
        piece = decay_all[:, s * half : (s + 1) * half]
        high, low = split(piece)
        message[s, 0:HALO, :] = jnp.concatenate(
            [high.astype(F32), low.astype(F32), jnp.zeros((HALO - 2, half), F32)], axis=0
        ).astype(BF16)
        for t in range(half // LANES):
            cols = pl.ds(s * half + t * LANES, LANES)
            for blk in range(1, count):
                added[blk, :, cols] = (
                    added[blk - 1, :, cols] * decays[blk : blk + 1, cols] + added[blk, :, cols]
                )
            message[s, HALO:, t * LANES : (t + 1) * LANES] = added[count - 1, :, cols].astype(BF16)

    partner = {"sp": pair * 2 + 1 - place}
    step_rows = STATE // CHUNKS
    first_copies, chain_copies, back_copies = [], [], []
    for i in range(CHUNKS):
        begin = 0 if i == 0 else HALO + i * step_rows
        size = HALO + step_rows if i == 0 else step_rows
        first_copies.append(
            pltpu.make_async_remote_copy(
                src_ref=message.at[1 - place, pl.ds(begin, size), :],
                dst_ref=pair_in.at[pl.ds(begin, size), :],
                send_sem=m1_send.at[i],
                recv_sem=m1_recv.at[i],
                device_id=partner,
                device_id_type=MESH,
            )
        )
        rows = pl.ds(i * step_rows, step_rows)
        chain_copies.append(
            pltpu.make_async_remote_copy(
                src_ref=state_out.at[rows, :],
                dst_ref=state_in.at[rows, :],
                send_sem=m2_send.at[i],
                recv_sem=m2_recv.at[i],
                device_id={"sp": jnp.where(sp + 2 < n, sp + 2, sp - 2)},
                device_id_type=MESH,
            )
        )
        back_copies.append(
            pltpu.make_async_remote_copy(
                src_ref=partner_out.at[rows, :],
                dst_ref=carried.at[place, rows, :],
                send_sem=m3_send.at[i],
                recv_sem=m3_recv.at[i],
                device_id=partner,
                device_id_type=MESH,
            )
        )
    for copy in first_copies:
        copy.start()

    per_group = heads // (shared // STATE)
    left = lax.broadcasted_iota(jnp.int32, (BLOCK, LANES), 1) < HEAD_DIM
    keep = ri >= ci

    @pl.loop(0, count)
    def _(blk):
        rows = pl.ds(pl.multiple_of(blk * BLOCK, BLOCK), BLOCK)
        for t in range(shared // LANES):
            conv_tile(blk, kc_ref, t * LANES, inner + shared)
        cum = cum_scr[rows, :]
        across = cum_t[blk]
        for g in range(shared // STATE):
            scores = lax.dot_general(
                act[rows, pl.ds(inner + shared + g * STATE, STATE)],
                act[rows, pl.ds(inner + g * STATE, STATE)],
                (((1,), (1,)), ((), ())),
                preferred_element_type=F32,
            )
            for h in range(g * per_group, (g + 1) * per_group, 2):
                mixes = []
                for k in (h, h + 1):
                    gap = jnp.where(keep, cum[:, k : k + 1] - across[k : k + 1, :], -jnp.inf)
                    mixes.append(
                        (scores * jnp.exp(gap) * across[heads + k : heads + k + 1, :]).astype(BF16)
                    )
                cols = pl.ds(h * HEAD_DIM, LANES)
                x_pair = act[rows, cols]
                zero = jnp.zeros_like(x_pair)
                stack = jnp.concatenate(
                    [jnp.where(left, x_pair, zero), jnp.where(left, zero, x_pair)], axis=0
                )
                y_diag[rows, cols] = jnp.dot(
                    jnp.concatenate(mixes, axis=1), stack, preferred_element_type=F32
                )
                gate_act[rows, cols] = silu(gate_ref[rows, cols].astype(F32))
        grown_high, grown_low = split(growth[rows, :])
        for t in range(inner // WIDE):
            cols = pl.ds(t * WIDE, WIDE)
            grown[rows, cols] = jnp.dot(
                grown_high, table[:, cols], preferred_element_type=F32
            ) + jnp.dot(grown_low, table[:, cols], preferred_element_type=F32)

    def decay_of(ref_rows):
        values = ref_rows.astype(F32)
        return values[0:1, :] + values[1:2, :]

    @pl.when(pair == 0)
    def _():
        state_in[...] = jnp.zeros_like(state_in)

    for i in range(CHUNKS):
        rows = pl.ds(i * step_rows, step_rows)
        from_rows = pl.ds(HALO + i * step_rows, step_rows)
        first_copies[i].wait_recv()
        if i == 0:
            own_decay = decay_of(message[place, 0:HALO, :])
            other_decay = decay_of(pair_in[0:HALO, :])
            decay_0 = jnp.where(place == 0, own_decay, other_decay)
            decay_1 = jnp.where(place == 0, other_decay, own_decay)
        own = message[place, from_rows, :].astype(F32)
        other = pair_in[from_rows, :].astype(F32)
        state_0 = jnp.where(place == 0, own, other)
        state_1 = jnp.where(place == 0, other, own)
        total = state_1 + decay_1 * state_0

        @pl.when(pair > 0)
        def _():
            chain_copies[i].wait_recv()

        entering = state_in[rows, :].astype(F32)

        @pl.when(pair + 1 < pairs)
        def _():
            state_out[rows, :] = (total + decay_1 * (decay_0 * entering)).astype(BF16)
            chain_copies[i].start()

        second = (state_0 + decay_0 * entering).astype(BF16)
        arrived = entering.astype(BF16)
        partner_out[rows, :] = jnp.where(place == 0, second, arrived)
        back_copies[i].start()
        carried[place, rows, :] = jnp.where(place == 0, arrived, second)

    for copy in back_copies:
        copy.wait_recv()
    loads[3].wait()

    wi = lax.broadcasted_iota(jnp.int32, (WIDE, WIDE), 0) // HEAD_DIM
    wj = lax.broadcasted_iota(jnp.int32, (WIDE, WIDE), 1) // HEAD_DIM
    same_head = jnp.where(wi == wj, 1.0, 0.0).astype(BF16)
    per = inner // (shared // STATE)
    for t in range(inner // WIDE):
        cols = pl.ds(t * WIDE, WIDE)
        s, offset = (t * WIDE) // half, (t * WIDE) % half
        g = (t * WIDE) // per
        state = carried[s, :, offset : offset + WIDE].astype(F32)
        gain = gain_ref[:, cols].astype(F32)
        for blk in range(count):
            rows = slice(blk * BLOCK, (blk + 1) * BLOCK)
            if blk == 0:
                entering = state
            else:
                prefix = decays[0:1, cols]
                for k in range(1, blk):
                    prefix = prefix * decays[k : k + 1, cols]
                entering = added[blk - 1, :, cols] + prefix * state
            read = jnp.dot(
                act[rows, pl.ds(inner + shared + g * STATE, STATE)],
                entering.astype(BF16),
                preferred_element_type=F32,
            )
            gated = (y_diag[rows, cols] + grown[rows, cols] * read) * gate_act[rows, cols]
            square = jnp.dot((gated * gated).astype(BF16), same_head, preferred_element_type=F32)
            normed[rows, cols] = (
                gated * lax.rsqrt(square * (1.0 / HEAD_DIM) + 1e-05) * gain
            ).astype(BF16)

    def tp_copy(i):
        return pltpu.make_async_remote_copy(
            src_ref=part_out.at[i],
            dst_ref=part_in.at[i],
            send_sem=tp_send.at[i],
            recv_sem=tp_recv.at[i],
            device_id={"tp": 1 - tp},
            device_id_type=MESH,
        )

    @pl.loop(0, pieces)
    def _(i):
        cols = pl.ds(pl.multiple_of(i * WIDE, WIDE), WIDE)
        there = pl.ds(pl.multiple_of((1 - tp) * rows_out, HALO), rows_out)
        part_out[i] = jnp.dot(
            normed[there, :], weight[:, cols], preferred_element_type=F32
        ).astype(BF16)
        tp_copy(i).start()

    @pl.loop(0, pieces)
    def _(i):
        cols = pl.ds(pl.multiple_of(i * WIDE, WIDE), WIDE)
        here = pl.ds(pl.multiple_of(tp * rows_out, HALO), rows_out)
        part = jnp.dot(normed[here, :], weight[:, cols], preferred_element_type=F32)
        tp_copy(i).wait_recv()
        out_ref[:, cols] = (part + part_in[i].astype(F32)).astype(BF16)

    @pl.loop(0, pieces)
    def _(i):
        tp_copy(i).wait_send()

    @pl.when(sp + 1 < n)
    def _():
        for copy in halos:
            copy.wait_send()

    @pl.when(pair + 1 < pairs)
    def _():
        for copy in chain_copies:
            copy.wait_send()

    for copy in first_copies + back_copies:
        copy.wait_send()


def body(
    n,
    gate_in,
    values_in,
    input_state_in,
    output_state_in,
    step_in,
    conv_x,
    conv_b,
    conv_c,
    dt_bias,
    decay_rate,
    log_decay_extra,
    out_gain,
    w_out,
):
    span, inner = gate_in.shape
    shared = input_state_in.shape[1]
    heads = step_in.shape[1]
    width = w_out.shape[1]
    half = inner // 2
    rows_out = span // 2
    count = span // BLOCK
    pieces = width // WIDE
    full = inner + 2 * shared
    vmem = pl.BlockSpec(memory_space=pltpu.VMEM)
    anywhere = pl.BlockSpec(memory_space=pl.ANY)
    dma = pltpu.SemaphoreType.DMA
    return pl.pallas_call(
        functools.partial(kernel, n),
        out_shape=jax.ShapeDtypeStruct((rows_out, width), BF16),
        in_specs=[vmem, anywhere, anywhere, anywhere] + [vmem] * 8 + [anywhere],
        out_specs=vmem,
        scratch_shapes=[
            pltpu.VMEM((HALO + span, full), BF16),
            pltpu.VMEM((span, full), BF16),
            pltpu.VMEM(w_out.shape, BF16),
            pltpu.VMEM((heads, inner), BF16),
            pltpu.VMEM((span, heads), F32),
            pltpu.VMEM((span, heads), F32),
            pltpu.VMEM((span, heads), F32),
            pltpu.VMEM((count, 2 * heads, BLOCK), F32),
            pltpu.VMEM((count, STATE, inner), F32),
            pltpu.VMEM((span, inner), F32),
            pltpu.VMEM((span, inner), F32),
            pltpu.VMEM((span, inner), F32),
            pltpu.VMEM((8, inner), F32),
            pltpu.VMEM((2, HALO + STATE, half), BF16),
            pltpu.VMEM((HALO + STATE, half), BF16),
            pltpu.VMEM((STATE, half), BF16),
            pltpu.VMEM((STATE, half), BF16),
            pltpu.VMEM((STATE, half), BF16),
            pltpu.VMEM((2, STATE, half), BF16),
            pltpu.VMEM((span, inner), BF16),
            pltpu.VMEM((pieces, rows_out, WIDE), BF16),
            pltpu.VMEM((pieces, rows_out, WIDE), BF16),
            dma((4,)),
            dma((3,)),
            dma((3,)),
            dma((CHUNKS,)),
            dma((CHUNKS,)),
            dma((CHUNKS,)),
            dma((CHUNKS,)),
            dma((CHUNKS,)),
            dma((CHUNKS,)),
            dma((pieces,)),
            dma((pieces,)),
        ],
        compiler_params=pltpu.CompilerParams(
            collective_id=0, has_side_effects=True, vmem_limit_bytes=56 * 1024 * 1024
        ),
    )(
        gate_in,
        values_in,
        input_state_in,
        output_state_in,
        step_in,
        conv_x,
        conv_b,
        conv_c,
        dt_bias.reshape(1, -1),
        decay_rate.reshape(1, -1),
        log_decay_extra,
        out_gain.reshape(1, -1),
        w_out,
    )


def solution(mesh):
    n = mesh.shape["sp"]
    placed = (
        P(("grp", "sp"), "tp"),
        P(("grp", "sp"), "tp"),
        P(("grp", "sp"), "tp"),
        P(("grp", "sp"), "tp"),
        P(("grp", "sp"), "tp"),
        P(None, "tp"),
        P(None, "tp"),
        P(None, "tp"),
        P("tp"),
        P("tp"),
        P(("grp", "sp"), "tp"),
        P("tp"),
        P("tp", None),
    )
    return jax.shard_map(
        functools.partial(body, n),
        mesh=mesh,
        in_specs=placed,
        out_specs=P(("grp", "sp", "tp"), None),
        check_vma=False,
    )
```

```python
import functools

import jax
import jax.numpy as jnp
from jax import lax
from jax.experimental import pallas as pl
from jax.experimental.pallas import tpu as pltpu
from jax.sharding import PartitionSpec as P

HEAD_DIM = 64
STATE = 128
CONV = 4
BLOCK = 128
HALO = 16
CHUNKS = 4
LANES = 128
WIDE = 256
MESH = pl.DeviceIdType.MESH
F32 = jnp.float32
BF16 = jnp.bfloat16


def silu(v):
    return v / (1.0 + jnp.exp(-v))


def split(v):
    high = v.astype(BF16)
    return high, (v - high.astype(F32)).astype(BF16)


def spread(v, table):
    high, low = split(v)
    return jnp.dot(high, table, preferred_element_type=F32) + jnp.dot(
        low, table, preferred_element_type=F32
    )


def kernel(
    n,
    gate_hbm,
    values_ref,
    b_ref,
    c_ref,
    step_ref,
    kx_ref,
    kb_ref,
    kc_ref,
    bias_ref,
    rate_ref,
    extra_ref,
    gain_ref,
    w_ref,
    out_ref,
    gate_ref,
    stage,
    act,
    weight,
    table,
    to_end,
    growth,
    cum_scr,
    cum_t,
    added,
    y_diag,
    gate_act,
    grown,
    decays,
    message,
    pair_in,
    state_in,
    state_out,
    partner_out,
    carried,
    normed,
    part_out,
    part_in,
    load_sem,
    halo_send,
    halo_recv,
    m1_send,
    m1_recv,
    m2_send,
    m2_recv,
    m3_send,
    m3_recv,
    tp_send,
    tp_recv,
):
    sp = lax.axis_index("sp")
    tp = lax.axis_index("tp")
    place = sp % 2
    pair = sp // 2
    pairs = n // 2
    span, inner = gate_hbm.shape
    shared = b_ref.shape[1]
    count = span // BLOCK
    heads = inner // HEAD_DIM
    half = inner // 2
    rows_out, width = out_ref.shape
    pieces = width // WIDE

    loads = [
        pltpu.make_async_copy(values_ref, stage.at[pl.ds(HALO, span), pl.ds(0, inner)], load_sem.at[0]),
        pltpu.make_async_copy(b_ref, stage.at[pl.ds(HALO, span), pl.ds(inner, shared)], load_sem.at[1]),
        pltpu.make_async_copy(
            c_ref, stage.at[pl.ds(HALO, span), pl.ds(inner + shared, shared)], load_sem.at[2]
        ),
        pltpu.make_async_copy(w_ref, weight, load_sem.at[3]),
        pltpu.make_async_copy(gate_hbm, gate_ref, load_sem.at[4]),
    ]
    for load in loads:
        load.start()

    barrier = pltpu.get_barrier_semaphore()
    for distance in (1, 2):

        @pl.when(sp >= distance)
        def _():
            pl.semaphore_signal(barrier, inc=1, device_id={"sp": sp - distance}, device_id_type=MESH)

        @pl.when(sp + distance < n)
        def _():
            pl.semaphore_signal(barrier, inc=1, device_id={"sp": sp + distance}, device_id_type=MESH)

    pl.semaphore_signal(barrier, inc=1, device_id={"tp": 1 - tp}, device_id_type=MESH)
    peers = 1
    for distance in (1, 2):
        peers = peers + jnp.where(sp >= distance, 1, 0) + jnp.where(sp + distance < n, 1, 0)
    pl.semaphore_wait(barrier, peers)

    halos = []
    for i, (source, start, size) in enumerate(
        ((values_ref, 0, inner), (b_ref, inner, shared), (c_ref, inner + shared, shared))
    ):
        halos.append(
            pltpu.make_async_remote_copy(
                src_ref=source.at[pl.ds(span - HALO, HALO), :],
                dst_ref=stage.at[pl.ds(0, HALO), pl.ds(start, size)],
                send_sem=halo_send.at[i],
                recv_sem=halo_recv.at[i],
                device_id={"sp": jnp.minimum(sp + 1, n - 1)},
                device_id_type=MESH,
            )
        )

    @pl.when(sp + 1 < n)
    def _():
        for copy in halos:
            copy.start()

    @pl.when(sp == 0)
    def _():
        stage[pl.ds(0, HALO), :] = jnp.zeros((HALO, stage.shape[1]), BF16)

    head_of = lax.broadcasted_iota(jnp.int32, (heads, inner), 1) // HEAD_DIM
    row_of = lax.broadcasted_iota(jnp.int32, (heads, inner), 0)
    table[...] = jnp.where(head_of == row_of, 1.0, 0.0).astype(BF16)
    ei = lax.broadcasted_iota(jnp.int32, (heads, heads), 0)
    ej = lax.broadcasted_iota(jnp.int32, (heads, heads), 1)
    bias = jnp.sum(jnp.where(ei == ej, bias_ref[...], 0.0), axis=1, keepdims=True)
    rate = jnp.sum(jnp.where(ei == ej, rate_ref[...], 0.0), axis=1, keepdims=True)
    step = jax.nn.softplus(step_ref[...].astype(F32) + bias)
    log_step = extra_ref[...] - step * rate
    ri = lax.broadcasted_iota(jnp.int32, (BLOCK, BLOCK), 0)
    ci = lax.broadcasted_iota(jnp.int32, (BLOCK, BLOCK), 1)
    upper = jnp.where(ri <= ci, 1.0, 0.0).astype(F32)
    totals = []
    for blk in range(count):
        rows = slice(blk * BLOCK, (blk + 1) * BLOCK)
        cum = jnp.dot(
            log_step[:, rows], upper, precision=lax.Precision.HIGHEST, preferred_element_type=F32
        )
        last = cum[:, BLOCK - 1 :]
        ends = jnp.exp(last - cum) * step[:, rows]
        rise = jnp.exp(cum)
        cum_t[blk] = jnp.concatenate([cum, step[:, rows]], axis=0)
        turned = jnp.concatenate(
            [cum, ends, rise, jnp.zeros((LANES - 3 * heads, BLOCK), F32)], axis=0
        ).T
        cum_scr[rows, :] = turned[:, :heads]
        to_end[rows, :] = turned[:, heads : 2 * heads]
        growth[rows, :] = turned[:, 2 * heads : 3 * heads]
        totals.append(turned[BLOCK - 1 :, 2 * heads : 3 * heads])
    stacked = jnp.concatenate(totals + [jnp.zeros((8 - count, heads), F32)], axis=0)
    decays[...] = spread(stacked, table[...])

    def conv_tile(blk, taps_ref, column, offset):
        rows = pl.ds(pl.multiple_of(blk * BLOCK, BLOCK), BLOCK + HALO)
        window = stage[rows, pl.ds(pl.multiple_of(offset + column, LANES), LANES)].astype(F32)
        taps = taps_ref[:, pl.ds(column, LANES)].astype(F32)
        total = taps[CONV - 1 :, :] * window[HALO:]
        for j in range(CONV - 1):
            total = total + taps[j : j + 1, :] * pltpu.roll(window, CONV - 1 - j, axis=0)[HALO:]
        out_rows = pl.ds(pl.multiple_of(blk * BLOCK, BLOCK), BLOCK)
        act[out_rows, pl.ds(pl.multiple_of(offset + column, LANES), LANES)] = silu(total).astype(BF16)

    def early(blk):
        rows = pl.ds(pl.multiple_of(blk * BLOCK, BLOCK), BLOCK)
        for t in range(shared // LANES):
            conv_tile(blk, kb_ref, t * LANES, inner)
        for t in range(inner // LANES):
            conv_tile(blk, kx_ref, t * LANES, 0)
        ends_high, ends_low = split(to_end[rows, :])
        per = inner // (shared // STATE)
        for g in range(shared // STATE):
            b_blk = act[rows, pl.ds(inner + g * STATE, STATE)].astype(F32).T.astype(BF16)
            for t in range(per // WIDE):
                cols = pl.ds(g * per + t * WIDE, WIDE)
                scale = jnp.dot(ends_high, table[:, cols], preferred_element_type=F32) + jnp.dot(
                    ends_low, table[:, cols], preferred_element_type=F32
                )
                weighted = (act[rows, cols].astype(F32) * scale).astype(BF16)
                added[blk, :, cols] = jnp.dot(b_blk, weighted, preferred_element_type=F32)

    for i in range(3):
        loads[i].wait()

    @pl.loop(0, count - 1)
    def _(i):
        early(count - 1 - i)

    @pl.when(sp > 0)
    def _():
        for copy in halos:
            copy.wait_recv()

    @pl.loop(0, 1)
    def _(i):
        early(i)

    decay_all = decays[0:1, :]
    for blk in range(1, count):
        decay_all = decay_all * decays[blk : blk + 1, :]
    for s in range(2):
        piece = decay_all[:, s * half : (s + 1) * half]
        high, low = split(piece)
        message[s, 0:HALO, :] = jnp.concatenate(
            [high.astype(F32), low.astype(F32), jnp.zeros((HALO - 2, half), F32)], axis=0
        ).astype(BF16)
        for t in range(half // LANES):
            cols = pl.ds(s * half + t * LANES, LANES)
            for blk in range(1, count):
                added[blk, :, cols] = (
                    added[blk - 1, :, cols] * decays[blk : blk + 1, cols] + added[blk, :, cols]
                )
            message[s, HALO:, t * LANES : (t + 1) * LANES] = added[count - 1, :, cols].astype(BF16)

    partner = {"sp": pair * 2 + 1 - place}
    step_rows = STATE // CHUNKS
    first_copies, chain_copies, back_copies = [], [], []
    for i in range(CHUNKS):
        begin = 0 if i == 0 else HALO + i * step_rows
        size = HALO + step_rows if i == 0 else step_rows
        first_copies.append(
            pltpu.make_async_remote_copy(
                src_ref=message.at[1 - place, pl.ds(begin, size), :],
                dst_ref=pair_in.at[pl.ds(begin, size), :],
                send_sem=m1_send.at[i],
                recv_sem=m1_recv.at[i],
                device_id=partner,
                device_id_type=MESH,
            )
        )
        rows = pl.ds(i * step_rows, step_rows)
        chain_copies.append(
            pltpu.make_async_remote_copy(
                src_ref=state_out.at[rows, :],
                dst_ref=state_in.at[rows, :],
                send_sem=m2_send.at[i],
                recv_sem=m2_recv.at[i],
                device_id={"sp": jnp.where(sp + 2 < n, sp + 2, sp - 2)},
                device_id_type=MESH,
            )
        )
        back_copies.append(
            pltpu.make_async_remote_copy(
                src_ref=partner_out.at[rows, :],
                dst_ref=carried.at[place, rows, :],
                send_sem=m3_send.at[i],
                recv_sem=m3_recv.at[i],
                device_id=partner,
                device_id_type=MESH,
            )
        )
    for copy in first_copies:
        copy.start()

    loads[4].wait()
    per_group = heads // (shared // STATE)
    left = lax.broadcasted_iota(jnp.int32, (BLOCK, LANES), 1) < HEAD_DIM
    keep = ri >= ci

    @pl.loop(0, count)
    def _(blk):
        rows = pl.ds(pl.multiple_of(blk * BLOCK, BLOCK), BLOCK)
        for t in range(shared // LANES):
            conv_tile(blk, kc_ref, t * LANES, inner + shared)
        cum = cum_scr[rows, :]
        across = cum_t[blk]
        for g in range(shared // STATE):
            scores = lax.dot_general(
                act[rows, pl.ds(inner + shared + g * STATE, STATE)],
                act[rows, pl.ds(inner + g * STATE, STATE)],
                (((1,), (1,)), ((), ())),
                preferred_element_type=F32,
            )
            for h in range(g * per_group, (g + 1) * per_group, 2):
                mixes = []
                for k in (h, h + 1):
                    gap = jnp.where(keep, cum[:, k : k + 1] - across[k : k + 1, :], -jnp.inf)
                    mixes.append(
                        (scores * jnp.exp(gap) * across[heads + k : heads + k + 1, :]).astype(BF16)
                    )
                cols = pl.ds(h * HEAD_DIM, LANES)
                x_pair = act[rows, cols]
                zero = jnp.zeros_like(x_pair)
                stack = jnp.concatenate(
                    [jnp.where(left, x_pair, zero), jnp.where(left, zero, x_pair)], axis=0
                )
                y_diag[rows, cols] = jnp.dot(
                    jnp.concatenate(mixes, axis=1), stack, preferred_element_type=F32
                )
                gate_act[rows, cols] = silu(gate_ref[rows, cols].astype(F32))
        grown_high, grown_low = split(growth[rows, :])
        for t in range(inner // WIDE):
            cols = pl.ds(t * WIDE, WIDE)
            grown[rows, cols] = jnp.dot(
                grown_high, table[:, cols], preferred_element_type=F32
            ) + jnp.dot(grown_low, table[:, cols], preferred_element_type=F32)

    def decay_of(ref_rows):
        values = ref_rows.astype(F32)
        return values[0:1, :] + values[1:2, :]

    @pl.when(pair == 0)
    def _():
        state_in[...] = jnp.zeros_like(state_in)

    for i in range(CHUNKS):
        rows = pl.ds(i * step_rows, step_rows)
        from_rows = pl.ds(HALO + i * step_rows, step_rows)
        first_copies[i].wait_recv()
        if i == 0:
            own_decay = decay_of(message[place, 0:HALO, :])
            other_decay = decay_of(pair_in[0:HALO, :])
            decay_0 = jnp.where(place == 0, own_decay, other_decay)
            decay_1 = jnp.where(place == 0, other_decay, own_decay)
        own = message[place, from_rows, :].astype(F32)
        other = pair_in[from_rows, :].astype(F32)
        state_0 = jnp.where(place == 0, own, other)
        state_1 = jnp.where(place == 0, other, own)
        total = state_1 + decay_1 * state_0

        @pl.when(pair > 0)
        def _():
            chain_copies[i].wait_recv()

        entering = state_in[rows, :].astype(F32)

        @pl.when(pair + 1 < pairs)
        def _():
            state_out[rows, :] = (total + decay_1 * (decay_0 * entering)).astype(BF16)
            chain_copies[i].start()

        second = (state_0 + decay_0 * entering).astype(BF16)
        arrived = entering.astype(BF16)
        partner_out[rows, :] = jnp.where(place == 0, second, arrived)
        back_copies[i].start()
        carried[place, rows, :] = jnp.where(place == 0, arrived, second)

    for copy in back_copies:
        copy.wait_recv()
    loads[3].wait()

    wi = lax.broadcasted_iota(jnp.int32, (WIDE, WIDE), 0) // HEAD_DIM
    wj = lax.broadcasted_iota(jnp.int32, (WIDE, WIDE), 1) // HEAD_DIM
    same_head = jnp.where(wi == wj, 1.0, 0.0).astype(BF16)
    per = inner // (shared // STATE)
    for t in range(inner // WIDE):
        cols = pl.ds(t * WIDE, WIDE)
        s, offset = (t * WIDE) // half, (t * WIDE) % half
        g = (t * WIDE) // per
        state = carried[s, :, offset : offset + WIDE].astype(F32)
        gain = gain_ref[cols].astype(F32).reshape(1, WIDE)
        for blk in range(count):
            rows = slice(blk * BLOCK, (blk + 1) * BLOCK)
            if blk == 0:
                entering = state
            else:
                prefix = decays[0:1, cols]
                for k in range(1, blk):
                    prefix = prefix * decays[k : k + 1, cols]
                entering = added[blk - 1, :, cols] + prefix * state
            read = jnp.dot(
                act[rows, pl.ds(inner + shared + g * STATE, STATE)],
                entering.astype(BF16),
                preferred_element_type=F32,
            )
            gated = (y_diag[rows, cols] + grown[rows, cols] * read) * gate_act[rows, cols]
            square = jnp.dot((gated * gated).astype(BF16), same_head, preferred_element_type=F32)
            normed[rows, cols] = (
                gated * lax.rsqrt(square * (1.0 / HEAD_DIM) + 1e-05) * gain
            ).astype(BF16)

    def tp_copy(i):
        return pltpu.make_async_remote_copy(
            src_ref=part_out.at[i],
            dst_ref=part_in.at[i],
            send_sem=tp_send.at[i],
            recv_sem=tp_recv.at[i],
            device_id={"tp": 1 - tp},
            device_id_type=MESH,
        )

    @pl.loop(0, pieces)
    def _(i):
        cols = pl.ds(pl.multiple_of(i * WIDE, WIDE), WIDE)
        there = pl.ds(pl.multiple_of((1 - tp) * rows_out, HALO), rows_out)
        part_out[i] = jnp.dot(
            normed[there, :], weight[:, cols], preferred_element_type=F32
        ).astype(BF16)
        tp_copy(i).start()

    @pl.loop(0, pieces)
    def _(i):
        cols = pl.ds(pl.multiple_of(i * WIDE, WIDE), WIDE)
        here = pl.ds(pl.multiple_of(tp * rows_out, HALO), rows_out)
        part = jnp.dot(normed[here, :], weight[:, cols], preferred_element_type=F32)
        tp_copy(i).wait_recv()
        out_ref[:, cols] = (part + part_in[i].astype(F32)).astype(BF16)

    @pl.loop(0, pieces)
    def _(i):
        tp_copy(i).wait_send()

    @pl.when(sp + 1 < n)
    def _():
        for copy in halos:
            copy.wait_send()

    @pl.when(pair + 1 < pairs)
    def _():
        for copy in chain_copies:
            copy.wait_send()

    for copy in first_copies + back_copies:
        copy.wait_send()


def body(
    n,
    gate_in,
    values_in,
    input_state_in,
    output_state_in,
    step_in,
    conv_x,
    conv_b,
    conv_c,
    dt_bias,
    decay_rate,
    log_decay_extra,
    out_gain,
    w_out,
):
    span, inner = gate_in.shape
    shared = input_state_in.shape[1]
    heads = step_in.shape[1]
    width = w_out.shape[1]
    half = inner // 2
    rows_out = span // 2
    count = span // BLOCK
    pieces = width // WIDE
    full = inner + 2 * shared
    vmem = pl.BlockSpec(memory_space=pltpu.VMEM)
    anywhere = pl.BlockSpec(memory_space=pl.ANY)
    dma = pltpu.SemaphoreType.DMA
    return pl.pallas_call(
        functools.partial(kernel, n),
        out_shape=jax.ShapeDtypeStruct((rows_out, width), BF16),
        in_specs=[anywhere, anywhere, anywhere, anywhere] + [vmem] * 8 + [anywhere],
        out_specs=vmem,
        scratch_shapes=[
            pltpu.VMEM((span, inner), BF16),
            pltpu.VMEM((HALO + span, full), BF16),
            pltpu.VMEM((span, full), BF16),
            pltpu.VMEM(w_out.shape, BF16),
            pltpu.VMEM((heads, inner), BF16),
            pltpu.VMEM((span, heads), F32),
            pltpu.VMEM((span, heads), F32),
            pltpu.VMEM((span, heads), F32),
            pltpu.VMEM((count, 2 * heads, BLOCK), F32),
            pltpu.VMEM((count, STATE, inner), F32),
            pltpu.VMEM((span, inner), F32),
            pltpu.VMEM((span, inner), F32),
            pltpu.VMEM((span, inner), F32),
            pltpu.VMEM((8, inner), F32),
            pltpu.VMEM((2, HALO + STATE, half), BF16),
            pltpu.VMEM((HALO + STATE, half), BF16),
            pltpu.VMEM((STATE, half), BF16),
            pltpu.VMEM((STATE, half), BF16),
            pltpu.VMEM((STATE, half), BF16),
            pltpu.VMEM((2, STATE, half), BF16),
            pltpu.VMEM((span, inner), BF16),
            pltpu.VMEM((pieces, rows_out, WIDE), BF16),
            pltpu.VMEM((pieces, rows_out, WIDE), BF16),
            dma((5,)),
            dma((3,)),
            dma((3,)),
            dma((CHUNKS,)),
            dma((CHUNKS,)),
            dma((CHUNKS,)),
            dma((CHUNKS,)),
            dma((CHUNKS,)),
            dma((CHUNKS,)),
            dma((pieces,)),
            dma((pieces,)),
        ],
        compiler_params=pltpu.CompilerParams(
            collective_id=0, has_side_effects=True, vmem_limit_bytes=56 * 1024 * 1024
        ),
    )(
        gate_in,
        values_in,
        input_state_in,
        output_state_in,
        step_in.T,
        conv_x,
        conv_b,
        conv_c,
        dt_bias.reshape(1, -1),
        decay_rate.reshape(1, -1),
        log_decay_extra.T,
        out_gain,
        w_out,
    )


def solution(mesh):
    n = mesh.shape["sp"]
    placed = (
        P(("grp", "sp"), "tp"),
        P(("grp", "sp"), "tp"),
        P(("grp", "sp"), "tp"),
        P(("grp", "sp"), "tp"),
        P(("grp", "sp"), "tp"),
        P(None, "tp"),
        P(None, "tp"),
        P(None, "tp"),
        P("tp"),
        P("tp"),
        P(("grp", "sp"), "tp"),
        P("tp"),
        P("tp", None),
    )
    return jax.shard_map(
        functools.partial(body, n),
        mesh=mesh,
        in_specs=placed,
        out_specs=P(("grp", "sp", "tp"), None),
        check_vma=False,
    )
```
